32 devices in a mesh: ep: 8 (over z, y), tp: 4 (over x, core).
Axes of the slice: x: 2, y: 2, z: 4, core: 2. Of those that a mesh axis runs over, the one named last changes fastest.
Arguments:
- tokens: bfloat16 [1024, 2048], P('ep'), may hold values from -6 to 6
- cotangent: bfloat16 [1024, 2048], P('ep'), may hold values from -2 to 2
- route_weights: float32 [1024, 2], P('ep'), may hold values from 0.25 to 2.5
- routes: int32 [1024, 2], P('ep'), may hold values from 0 to 7, all different within a row; in each aligned block of 128 rows (0 to 127, 128 to 255, ...) at most 64 rows name the same one
- gate_proj: bfloat16 [8, 2048, 512], P('ep', None, 'tp'), may hold values from -0.125 to 0.125
- up_proj: bfloat16 [8, 2048, 512], P('ep', None, 'tp'), may hold values from -0.125 to 0.125
- down_proj: bfloat16 [8, 512, 2048], P('ep', 'tp'), may hold values from -0.25 to 0.25
- shared_down: bfloat16 [2048, 512], P(None, 'tp'), may hold values from -0.25 to 0.25
- shared_hidden: bfloat16 [1024, 512], P('ep', 'tp'), may hold values from -0.29882812 to 0.29882812
Outputs:
- tokens_grad: bfloat16 [1024, 2048], P('ep', 'tp')
- weights_grad: float32 [1024, 2], P('ep')
- gate_proj_grad: bfloat16 [8, 2048, 512], P('ep', None, 'tp')
- up_proj_grad: bfloat16 [8, 2048, 512], P('ep', None, 'tp')
- down_proj_grad: bfloat16 [8, 512, 2048], P('ep', 'tp')
- hidden_grad: bfloat16 [1024, 512], P('ep', 'tp')
- shared_grad: float32 [2048, 512], P('ep', 'tp')
The draws below stay inside these ranges and needn't reach their ends.
Inputs may be any that keep to these rules, and one draw needn't show every extreme that they name: `routes`: in each aligned block of 128 rows no expert is named more than 64 times, a bound that some block reaches; the 2 experts of a row differ.
All inputs are finite; a program needn't handle non-finite values.
Results may differ from the reference program's by a relative error of at most 0.012.
Values may be sent and summed in bfloat16 or wider, within the bound.
A program may use at most 64 MiB of HBM per device.

```python
import math
import jax
import jax.numpy as jnp
import numpy as np
from jax import lax

D = 2048
FF = 512
D_SHARED = 512
TOP = 2
TOK_DEV = 128
EXPERTS = 8
TOKENS = 1024
CAP = 64
N_EP = 8
N_TP = 4


def raised(values, stream_key, source, target, parts, factor):
    def block_of(position):
        return (jnp.arange(values.shape[position]) // (values.shape[position] // parts)).reshape((-1,) + (1,) * (values.ndim - 1 - position))

    near = jax.random.permutation(stream_key, parts)[block_of(target)]
    other_side = (block_of(target) + parts // 2) % parts
    return jnp.where((block_of(source) == near) | (block_of(source) == other_side), factor * values, values)


def block_levels(stream_key, extent, shards, low, top_value):
    factor_of, own = 1.0, jax.random.fold_in(stream_key, 6)
    for axis_at, shards_of in shards:
        draws = jnp.exp(jax.random.uniform(jax.random.fold_in(own, axis_at), (shards_of,), jnp.float32, low / len(shards), top_value / len(shards)))
        factor_of = factor_of * jnp.repeat(draws, extent[axis_at] // shards_of).reshape([-1 if axis == axis_at else 1 for axis in range(len(extent))])
    return factor_of


def assign_block(rng, own, number, rows, count, top, limit, lean):
    sequence = jax.random.permutation(rng, count)
    heavy_load, common = load_shares(count, rows * top, limit, lean, True), load_shares(count, rows * top, limit, lean, False)
    places = jnp.arange(count)

    def named(sizes, turn):
        used = int((sizes > 0).sum())
        fixed = max(1, used // 4)
        passed = fixed + (places - fixed + turn * (used - fixed)) % max(1, count - fixed)
        return jnp.zeros((count,), jnp.int32).at[sequence[jnp.where(places < fixed, places, passed)]].set(jnp.asarray(sizes, jnp.int32))

    sizes = jnp.where(number % 4 == 0, named(heavy_load, number // 4), named(common, number - number // 4 - 1))
    mixed = jax.random.permutation(jax.random.fold_in(own, 3), count)
    donor, sink = mixed[0:count // 2 * 2:2], mixed[1:count // 2 * 2:2]
    margin = jnp.minimum(sizes[donor] - 1, limit - sizes[sink]) // 2
    margin = jnp.where((donor == sequence[0]) | (sink == sequence[0]) | (sizes[sink] == 0), 0, jnp.maximum(margin, 0))
    passed = jax.random.randint(jax.random.fold_in(own, 4), (count // 2,), 0, 1 << 20) % (margin + 1)
    sizes = sizes.at[donor].add(-passed).at[sink].add(passed)
    items = jnp.searchsorted(jnp.cumsum(sizes), jnp.arange(rows * top), side="right").astype(jnp.int32)
    grid = items.reshape(top, rows).T
    grid = grid[jax.random.permutation(jax.random.fold_in(own, 1), rows)]
    turn = jax.random.randint(jax.random.fold_in(own, 2), (rows, 1), 0, top)
    return jnp.take_along_axis(grid, (jnp.arange(top)[None, :] + turn) % top, axis=1)


def load_shares(number_of, total, limit, lean, full):
    loads = [(1 << 20) // math.isqrt(rank ** lean) + 1 for rank in range(1, number_of + 1)]
    largest = limit if full else min(limit, max(-(-total // number_of), total * loads[0] // sum(loads)))
    least = 1 if total - largest >= number_of - 1 else 0
    counts, spare = [largest] + [least] * (number_of - 1), total - largest - least * (number_of - 1)
    while spare > 0:
        free = [i for i in range(1, number_of) if counts[i] < largest] or [i for i in range(1, number_of) if counts[i] < limit]
        mass, budget = sum([loads[i] for i in free]), spare
        for i in free:
            extra = min(limit - counts[i], max(1, budget * loads[i] // mass), spare)
            counts[i] = counts[i] + extra
            spare = spare - extra
    return np.array(counts)


def centred(own_key, shape, spread, limit, shards=(), kind=jnp.bfloat16):
    result = spread * jax.random.normal(own_key, shape, jnp.float32)
    if shards:
        result = result * block_levels(own_key, shape, shards, -0.22, 0.18)
    return jnp.clip(result, -limit, limit).astype(kind)


def noise_with(rng, extent, scale, most, split, heavy, kind=jnp.bfloat16):
    drawn = scale * jax.random.normal(rng, extent, jnp.float32)
    if split:
        drawn = drawn * block_levels(rng, extent, split, -0.22, 0.18)
    return jnp.clip(raised(drawn, jax.random.fold_in(rng, 3), *heavy), -most, most).astype(kind)


def setup_inputs(seed: int = 0) -> dict:
    seeds = jax.random.split(jax.random.key(seed), 10)
    tokens = centred(seeds[0], (TOKENS, D), 1.0, 6.0, ((0, 8),))
    cotangent = noise_with(seeds[1], (TOKENS, D), 0.25, 2.0, ((0, 8),), (0, 1, 8, 2.0))
    route_weights = jnp.clip(jnp.exp(math.log(2.5) - 2.3025851 * jax.random.uniform(seeds[2], (TOKENS, TOP), jnp.float32) ** block_levels(seeds[2], (TOKENS, TOP), ((0, 8),), -0.2, 0.2)), 0.25, 2.5)
    routes_keys = jax.random.split(jax.random.fold_in(seeds[3], 1), TOKENS // TOK_DEV)
    routes_turns = jax.random.permutation(jax.random.fold_in(seeds[3], 3), TOKENS // TOK_DEV)
    routes = jax.vmap(lambda own, number: assign_block(jax.random.fold_in(seeds[3], 2), own, number, TOK_DEV, EXPERTS, TOP, CAP, 2))(routes_keys, routes_turns).reshape((TOKENS, TOP))
    gate_proj = centred(seeds[4], (EXPERTS, D, FF), D ** -0.5, 0.125, ((0, 8), (2, 4)))
    up_proj = centred(seeds[5], (EXPERTS, D, FF), D ** -0.5, 0.125, ((0, 8), (2, 4)))
    down_proj = centred(seeds[6], (EXPERTS, FF, D), FF ** -0.5, 0.25, ((0, 8), (1, 4)))
    shared_down = centred(seeds[7], (D, D_SHARED), D_SHARED ** -0.5, 0.25, ((1, 4),))
    shared_hidden = centred(seeds[8], (TOKENS, D_SHARED), 0.05, 0.29882812, ((0, 8), (1, 4)))
    return {"tokens": tokens, "cotangent": cotangent, "route_weights": route_weights, "routes": routes, "gate_proj": gate_proj, "up_proj": up_proj, "down_proj": down_proj, "shared_down": shared_down, "shared_hidden": shared_hidden}


def slot_index(routes):
    blocks = routes.reshape(N_EP, TOK_DEV * TOP)
    one_hot = (blocks[:, :, None] == jnp.arange(EXPERTS, dtype=jnp.int32)[None, None, :]).astype(jnp.int32)
    earlier = jnp.cumsum(one_hot, axis=1) - one_hot
    rank_in = jnp.sum(earlier * one_hot, axis=2)
    source = jnp.arange(N_EP, dtype=jnp.int32)[:, None]
    return ((blocks * N_EP + source) * CAP + rank_in).astype(jnp.int32)


def one_expert(inputs):
    in_rows, in_grads, in_weights, w_gate, w_up, w_down = inputs
    gate = jnp.dot(in_rows, w_gate, preferred_element_type=jnp.float32)
    upper = jnp.dot(in_rows, w_up, preferred_element_type=jnp.float32)
    active = jax.nn.silu(gate)
    hidden = (active * upper).astype(jnp.bfloat16)
    backed = jnp.dot(in_grads, w_down.T, preferred_element_type=jnp.float32)
    gate_grad = jnp.sum(hidden.astype(jnp.float32) * backed, axis=1).astype(jnp.bfloat16)
    weight_col = in_weights.astype(jnp.float32)[:, None]
    d_hidden = weight_col * backed
    sigma = jax.nn.sigmoid(gate)
    d_gate = (d_hidden * upper * sigma * (1.0 + gate * (1.0 - sigma))).astype(jnp.bfloat16)
    d_up = (d_hidden * active).astype(jnp.bfloat16)
    scaled = (weight_col * in_grads.astype(jnp.float32)).astype(jnp.bfloat16)
    down_grad = jnp.dot(hidden.T, scaled, preferred_element_type=jnp.float32).astype(jnp.bfloat16)
    gate_wgrad = jnp.dot(in_rows.T, d_gate, preferred_element_type=jnp.float32).astype(jnp.bfloat16)
    up_wgrad = jnp.dot(in_rows.T, d_up, preferred_element_type=jnp.float32).astype(jnp.bfloat16)
    block_units = FF // N_TP
    slot_count = in_rows.shape[0]
    dg_blocks = d_gate.astype(jnp.float32).reshape(slot_count, N_TP, block_units)
    du_blocks = d_up.astype(jnp.float32).reshape(slot_count, N_TP, block_units)
    wg_blocks = w_gate.astype(jnp.float32).reshape(D, N_TP, block_units)
    wu_blocks = w_up.astype(jnp.float32).reshape(D, N_TP, block_units)
    partial_value = jnp.einsum("rtf,dtf->trd", dg_blocks, wg_blocks) + jnp.einsum("rtf,dtf->trd", du_blocks, wu_blocks)
    partial_value = lax.optimization_barrier(partial_value.astype(jnp.bfloat16))
    input_grad = jnp.sum(partial_value.astype(jnp.float32), axis=0).astype(jnp.bfloat16)
    return input_grad, gate_grad, gate_wgrad, up_wgrad, down_grad


def reference(tokens, cotangent, route_weights, routes, gate_proj, up_proj, down_proj, shared_down, shared_hidden):
    slot_ids = slot_index(routes).reshape(-1)
    owner_ids = jnp.arange(TOKENS * TOP, dtype=jnp.int32) // TOP
    total_slots = EXPERTS * N_EP * CAP
    per_expert = N_EP * CAP
    row_buf = jnp.zeros((total_slots, D), jnp.bfloat16).at[slot_ids].set(tokens[owner_ids])
    grad_buf = jnp.zeros((total_slots, D), jnp.bfloat16).at[slot_ids].set(cotangent[owner_ids])
    weight_buf = jnp.zeros((total_slots,), jnp.bfloat16).at[slot_ids].set(route_weights.reshape(-1).astype(jnp.bfloat16))
    results = lax.map(one_expert, (row_buf.reshape(EXPERTS, per_expert, D), grad_buf.reshape(EXPERTS, per_expert, D),
                                   weight_buf.reshape(EXPERTS, per_expert), gate_proj, up_proj, down_proj))
    input_grad, gate_grad, gate_wgrad, up_wgrad, down_grad = results
    picked = input_grad.reshape(total_slots, D)[slot_ids].reshape(TOKENS, TOP, D)
    tokens_grad = jnp.sum(picked.astype(jnp.float32), axis=1).astype(jnp.bfloat16)
    weights_grad = gate_grad.reshape(total_slots)[slot_ids].astype(jnp.float32).reshape(TOKENS, TOP)
    hidden_grad = jnp.dot(cotangent, shared_down, preferred_element_type=jnp.float32).astype(jnp.bfloat16)
    shared_grad = jnp.dot(cotangent.T, shared_hidden, preferred_element_type=jnp.float32)
    return tokens_grad, weights_grad, gate_wgrad, up_wgrad, down_grad, hidden_grad, shared_grad
```

```python
import functools

import jax
import jax.numpy as jnp
from jax import lax
from jax.experimental import pallas as pl
from jax.experimental.pallas import tpu as pltpu
from jax.sharding import PartitionSpec as P

MESH = pl.DeviceIdType.MESH
BF = jnp.bfloat16
F32 = jnp.float32
DISP, WGT, FWD_X, FWD_C, FWD_XC, RET_C, RET_X, RET_EP, RET_G, SHARE, GSUM = range(11)


def dot_f32(a, b, dims):
    return lax.dot_general(a, b, (dims, ((), ())), preferred_element_type=F32)


def kernel(
    n,
    cap,
    tok_ref,
    cot_ref,
    rw_ref,
    rt_ref,
    wg_ref,
    wu_ref,
    wd_ref,
    sd_ref,
    sh_ref,
    otok_ref,
    ow_ref,
    og_ref,
    ou_ref,
    od_ref,
    ohid_ref,
    osh_ref,
    perm,
    sbuf,
    abuf,
    wsend,
    wrecv,
    wgu,
    hw,
    dgu,
    part,
    crecv,
    keep,
    xsend,
    xrecv,
    rsend,
    ret,
    gpart,
    gcore,
    gtwo,
    gx,
    gsend,
    gret,
    ssend,
    srecv,
    send_sem,
    recv_sem,
):
    me = lax.axis_index("ep")
    tp = lax.axis_index("tp")
    tok_rows, feat = tok_ref.shape
    top = rt_ref.shape[1]
    quarter = feat // 4
    units = wg_ref.shape[1]
    core_of = lax.rem(tp, 2)
    half_of = tp // 2
    tp_c = half_of * 2 + (1 - core_of)
    tp_x = (1 - half_of) * 2 + core_of
    tp_xc = (1 - half_of) * 2 + (1 - core_of)

    def copy(kind, at, src_ref, dst_ref, ep_to, tp_to):
        return pltpu.make_async_remote_copy(
            src_ref=src_ref,
            dst_ref=dst_ref,
            send_sem=send_sem.at[kind, at],
            recv_sem=recv_sem.at[kind, at],
            device_id=(ep_to, tp_to),
            device_id_type=MESH,
        )

    barrier = pltpu.get_barrier_semaphore()
    for d in range(1, n):
        pl.semaphore_signal(
            barrier, inc=1, device_id=(lax.rem(me + d, n), tp), device_id_type=MESH
        )
    for other in (tp_c, tp_x):
        pl.semaphore_signal(barrier, inc=1, device_id=(me, other), device_id_type=MESH)

    lane = lax.broadcasted_iota(jnp.int32, (tok_rows, 128), 1)
    named = jnp.zeros((tok_rows, 128), F32)
    weight_of = jnp.zeros((tok_rows, 128), F32)
    for k in range(top):
        hit = rt_ref[:, k : k + 1] == lane
        named = named + jnp.where(hit, 1.0, 0.0)
        weight_of = weight_of + jnp.where(hit, rw_ref[:, k : k + 1].astype(BF).astype(F32), 0.0)
    named_t = named.T
    weight_t = weight_of.T
    before = lax.broadcasted_iota(jnp.int32, (tok_rows, tok_rows), 0) < lax.broadcasted_iota(
        jnp.int32, (tok_rows, tok_rows), 1
    )
    rank_t = dot_f32(named_t.astype(BF), jnp.where(before, 1.0, 0.0).astype(BF), ((1,), (0,)))
    slot = lax.broadcasted_iota(jnp.int32, (cap, tok_rows), 0).astype(F32)
    wsend[...] = jnp.zeros_like(wsend)
    gpart[...] = jnp.zeros_like(gpart)
    for e in range(n):
        pick = jnp.where(slot == rank_t[e : e + 1, :], named_t[e : e + 1, :], 0.0).astype(BF)
        perm[e] = pick
        wrow = jnp.broadcast_to(weight_t[e : e + 1, :], (8, tok_rows)).astype(BF)
        wsend[e, :, 0:cap] = dot_f32(wrow, pick, ((1,), (1,)))
    every = perm[...].reshape(n * cap, tok_rows)
    cols = pl.ds(pl.multiple_of(tp * quarter, quarter), quarter)
    sbuf[:, 0] = dot_f32(every, tok_ref[:, cols], ((1,), (0,))).astype(BF).reshape(n, cap, quarter)
    sbuf[:, 1] = dot_f32(every, cot_ref[:, cols], ((1,), (0,))).astype(BF).reshape(n, cap, quarter)

    pl.semaphore_wait(barrier, n + 1)

    def disp(d):
        to = lax.rem(me + d, n)
        return copy(DISP, d, sbuf.at[to], abuf.at[me, tp], to, tp)

    def disp_w(d):
        to = lax.rem(me + d, n)
        return copy(WGT, d, wsend.at[to], wrecv.at[me], to, tp)

    def disp_in(d):
        of = lax.rem(me + n - d, n)
        return copy(DISP, d, abuf.at[of, tp], abuf.at[of, tp], of, tp)

    def disp_w_in(d):
        of = lax.rem(me + n - d, n)
        return copy(WGT, d, wrecv.at[of], wrecv.at[of], of, tp)

    def fwd(kind, d, block, to):
        of = lax.rem(me + n - d, n)
        return copy(kind, d, abuf.at[of, block], abuf.at[of, block], me, to)

    abuf[me, tp] = sbuf[me]
    wrecv[me] = wsend[me]

    @pl.loop(1, n)
    def _(d):
        disp(d).start()
        disp_w(d).start()

    fwd(FWD_X, 0, tp, tp_x).start()
    fwd(FWD_C, 0, tp, tp_c).start()

    wgu[:, 0:units] = wg_ref[...]
    wgu[:, units : 2 * units] = wu_ref[...]
    ohid_ref[...] = dot_f32(cot_ref[...], sd_ref[...], ((1,), (0,))).astype(BF)
    rows_each = feat // n
    for j in range(n):
        ssend[j] = dot_f32(
            cot_ref[:, j * rows_each : (j + 1) * rows_each], sh_ref[...], ((0,), (0,))
        ).astype(BF)

    @pl.loop(1, n)
    def _(d):
        disp_in(d).wait_recv()
        fwd(FWD_X, d, tp, tp_x).start()
        fwd(FWD_C, d, tp, tp_c).start()

        @pl.when(d >= 2)
        def _():
            fwd(FWD_X, d - 2, tp_x, tp_x).wait_recv()
            fwd(FWD_XC, d - 2, tp_x, tp_c).start()

    @pl.loop(1, n)
    def _(d):
        disp_w_in(d).wait_recv()
        disp(d).wait_send()
        disp_w(d).wait_send()

    def share(d):
        to = lax.rem(me + d, n)
        return copy(SHARE, d, ssend.at[to], srecv.at[me], to, tp)

    def share_in(d):
        of = lax.rem(me + n - d, n)
        return copy(SHARE, d, srecv.at[of], srecv.at[of], of, tp)

    srecv[me] = ssend[me]

    @pl.loop(1, n)
    def _(d):
        share(d).start()

    eye = lax.broadcasted_iota(jnp.int32, (cap, cap), 0) == lax.broadcasted_iota(
        jnp.int32, (cap, cap), 1
    )

    def to_core(d):
        of = lax.rem(me + n - d, n)
        return copy(RET_C, d, part.at[of, 1 - core_of], crecv.at[of], me, tp_c)

    @pl.loop(0, n)
    def _(d):
        of = lax.rem(me + n - d, n)

        @pl.when(d >= n - 2)
        def _():
            fwd(FWD_X, d, tp_x, tp_x).wait_recv()
            fwd(FWD_XC, d, tp_x, tp_c).start()

        fwd(FWD_C, d, tp_c, tp_c).wait_recv()
        fwd(FWD_XC, d, tp_xc, tp_c).wait_recv()
        both = jnp.zeros((cap, 2 * units), F32)
        backed = jnp.zeros((cap, units), F32)
        for b in range(4):
            at = slice(b * quarter, (b + 1) * quarter)
            both = both + dot_f32(abuf[of, b, 0], wgu[at, :], ((1,), (0,)))
            backed = backed + dot_f32(abuf[of, b, 1], wd_ref[:, at], ((1,), (1,)))
        gate = both[:, 0:units]
        upper = both[:, units : 2 * units]
        sigma = jax.nn.sigmoid(gate)
        active = gate * sigma
        hidden = (active * upper).astype(BF).astype(F32)
        wcol = jnp.sum(jnp.where(eye, wrecv[of, 0:1, 0:cap], 0.0), axis=1, keepdims=True)
        d_hidden = wcol * backed
        hw[of] = (wcol * hidden).astype(BF)
        d_both = jnp.concatenate(
            [
                (d_hidden * upper * sigma * (1.0 + gate * (1.0 - sigma))).astype(BF),
                (d_hidden * active).astype(BF),
            ],
            axis=1,
        )
        dgu[of] = d_both
        gpart[of, :, 0:cap] = lax.dot_general(
            jnp.ones((8, units), F32),
            hidden * backed,
            (((1,), (1,)), ((), ())),
            precision=lax.Precision.HIGHEST,
            preferred_element_type=F32,
        )
        for b in range(4):
            at = slice(b * quarter, (b + 1) * quarter)
            part[of, b % 2, b // 2] = dot_f32(d_both, wgu[at, :], ((1,), (1,))).astype(BF)
        to_core(d).start()

    def gate_copy(at, src_ref, dst_ref, to):
        return copy(GSUM, at, src_ref, dst_ref, me, to)

    gate_copy(0, gpart, gcore, tp_c).start()

    def to_x(d):
        of = lax.rem(me + n - d, n)
        return copy(RET_X, d, xsend.at[of], xrecv.at[of], me, tp_x)

    @pl.loop(0, n)
    def _(d):
        of = lax.rem(me + n - d, n)
        to_core(d).wait_recv()
        xsend[of] = (
            part[of, core_of, 1 - half_of].astype(F32) + crecv[of, 1 - half_of].astype(F32)
        ).astype(BF)
        to_x(d).start()
        keep[of] = part[of, core_of, half_of].astype(F32) + crecv[of, half_of].astype(F32)

    gate_copy(0, gpart, gcore, tp_c).wait()
    gtwo[...] = gpart[...] + gcore[...]
    gate_copy(1, gtwo, gx, tp_x).start()

    d_all = dgu[...].reshape(n * cap, 2 * units)
    h_all = hw[...].reshape(n * cap, units)
    for b in range(4):
        at = slice(b * quarter, (b + 1) * quarter)
        grad = dot_f32(abuf[:, b, 0].reshape(n * cap, quarter), d_all, ((0,), (0,))).astype(BF)
        og_ref[at, :] = grad[:, 0:units]
        ou_ref[at, :] = grad[:, units : 2 * units]
        od_ref[:, at] = dot_f32(
            h_all, abuf[:, b, 1].reshape(n * cap, quarter), ((0,), (0,))
        ).astype(BF)

    gate_copy(1, gtwo, gx, tp_x).wait()
    gsend[...] = gtwo[...] + gx[...]
    gret[me] = gsend[me]

    def back(d):
        to = lax.rem(me + d, n)
        return copy(RET_EP, d, rsend.at[to], ret.at[me], to, tp)

    def back_g(d):
        to = lax.rem(me + d, n)
        return copy(RET_G, d, gsend.at[to], gret.at[me], to, tp)

    def back_in(d):
        of = lax.rem(me + n - d, n)
        return copy(RET_EP, d, ret.at[of], ret.at[of], of, tp)

    def back_g_in(d):
        of = lax.rem(me + n - d, n)
        return copy(RET_G, d, gret.at[of], gret.at[of], of, tp)

    @pl.loop(1, n)
    def _(d):
        back_g(d).start()

    @pl.loop(0, n)
    def _(d):
        of = lax.rem(me + n - d, n)
        to_x(d).wait_recv()
        total = (keep[of] + xrecv[of].astype(F32)).astype(BF)

        @pl.when(d == 0)
        def _():
            ret[me] = total

        @pl.when(d > 0)
        def _():
            rsend[of] = total
            back(lax.rem(n - d, n)).start()

    @pl.loop(1, n)
    def _(d):
        share_in(d).wait_recv()
        back_g_in(d).wait_recv()

    sums = srecv[0].astype(F32)
    for j in range(1, n):
        sums = sums + srecv[j].astype(F32)
    osh_ref[...] = sums

    pieces = []
    for e in range(n):
        row = gret[e, :, 0:cap].astype(BF)
        pieces.append(dot_f32(row, perm[e], ((1,), (0,)))[0:1, :])
    pieces.append(jnp.zeros((128 - n, tok_rows), F32))
    values = jnp.concatenate(pieces, axis=0).T
    for k in range(top):
        hit = rt_ref[:, k : k + 1] == lane
        ow_ref[:, k : k + 1] = jnp.sum(jnp.where(hit, values, 0.0), axis=1, keepdims=True)

    @pl.loop(1, n)
    def _(d):
        back_in(d).wait_recv()

    otok_ref[...] = dot_f32(
        perm[...].reshape(n * cap, tok_rows), ret[...].reshape(n * cap, quarter), ((0,), (0,))
    ).astype(BF)

    @pl.loop(0, n)
    def _(d):
        fwd(FWD_X, d, tp, tp_x).wait_send()
        fwd(FWD_C, d, tp, tp_c).wait_send()
        fwd(FWD_XC, d, tp_x, tp_c).wait_send()
        to_core(d).wait_send()
        to_x(d).wait_send()

    @pl.loop(1, n)
    def _(d):
        share(d).wait_send()
        back(d).wait_send()
        back_g(d).wait_send()


def fused_shards(
    tokens,
    cotangent,
    route_weights,
    routes,
    gate_proj,
    up_proj,
    down_proj,
    shared_down,
    shared_hidden,
):
    n = lax.axis_size("ep")
    tok_rows, feat = tokens.shape
    units = gate_proj.shape[2]
    hid = shared_hidden.shape[1]
    cap = 2 * tok_rows * routes.shape[1] // n
    quarter = feat // 4
    out_shape = (
        jax.ShapeDtypeStruct((tok_rows, quarter), BF),
        jax.ShapeDtypeStruct(routes.shape, F32),
        jax.ShapeDtypeStruct((feat, units), BF),
        jax.ShapeDtypeStruct((feat, units), BF),
        jax.ShapeDtypeStruct((units, feat), BF),
        jax.ShapeDtypeStruct((tok_rows, hid), BF),
        jax.ShapeDtypeStruct((feat // n, hid), F32),
    )
    tiles = pltpu.VMEM((n, 8, 128), F32)
    outs = pl.pallas_call(
        functools.partial(kernel, n, cap),
        out_shape=out_shape,
        in_specs=[pl.BlockSpec(memory_space=pltpu.VMEM)] * 9,
        out_specs=tuple([pl.BlockSpec(memory_space=pltpu.VMEM)] * 7),
        scratch_shapes=[
            pltpu.VMEM((n, cap, tok_rows), BF),
            pltpu.VMEM((n, 2, cap, quarter), BF),
            pltpu.VMEM((n, 4, 2, cap, quarter), BF),
            tiles,
            tiles,
            pltpu.VMEM((feat, 2 * units), BF),
            pltpu.VMEM((n, cap, units), BF),
            pltpu.VMEM((n, cap, 2 * units), BF),
            pltpu.VMEM((n, 2, 2, cap, quarter), BF),
            pltpu.VMEM((n, 2, cap, quarter), BF),
            pltpu.VMEM((n, cap, quarter), F32),
            pltpu.VMEM((n, cap, quarter), BF),
            pltpu.VMEM((n, cap, quarter), BF),
            pltpu.VMEM((n, cap, quarter), BF),
            pltpu.VMEM((n, cap, quarter), BF),
            tiles,
            tiles,
            tiles,
            tiles,
            tiles,
            tiles,
            pltpu.VMEM((n, feat // n, hid), BF),
            pltpu.VMEM((n, feat // n, hid), BF),
            pltpu.SemaphoreType.DMA((11, n)),
            pltpu.SemaphoreType.DMA((11, n)),
        ],
        compiler_params=pltpu.CompilerParams(
            collective_id=0, has_side_effects=True, vmem_limit_bytes=60 * 1024 * 1024
        ),
    )(
        tokens,
        cotangent,
        route_weights,
        routes,
        gate_proj[0],
        up_proj[0],
        down_proj[0],
        shared_down,
        shared_hidden,
    )
    return outs[0], outs[1], outs[2][None], outs[3][None], outs[4][None], outs[5], outs[6]


def shards(*args):
    tokens, routes, gate_proj = args[0], args[3], args[4]
    n = lax.axis_size("ep")
    tok_rows, feat = tokens.shape
    fits = (
        gate_proj.shape[0] == 1
        and lax.axis_size("tp") == 4
        and tok_rows == 128
        and n <= 16
        and (2 * tok_rows * routes.shape[1]) % (16 * n) == 0
        and 2 * tok_rows * routes.shape[1] // n <= 128
        and feat % 512 == 0
        and feat // n % 128 == 0
    )
    if fits:
        return fused_shards(*args)
    return plain_shards(*args)


def plain_shards(
    tokens,
    cotangent,
    route_weights,
    routes,
    gate_proj,
    up_proj,
    down_proj,
    shared_down,
    shared_hidden,
):
    tok_rows, feat_width = tokens.shape
    top_count = routes.shape[1]
    exp_local = gate_proj.shape[0]
    ep_size = lax.axis_size("ep")
    tp_size = lax.axis_size("tp")
    exp_total = exp_local * ep_size
    capacity = 2 * tok_rows * top_count // exp_total
    quarter = feat_width // tp_size
    filled = exp_total * capacity
    flat_routes = routes.reshape(-1)
    one_hot = (flat_routes[:, None] == jnp.arange(exp_total, dtype=jnp.int32)[None, :]).astype(
        jnp.int32
    )
    rank_in = jnp.sum((jnp.cumsum(one_hot, axis=0) - one_hot) * one_hot, axis=1)
    slot_ids = flat_routes * capacity + rank_in
    route_owner = jnp.arange(flat_routes.shape[0], dtype=jnp.int32) // top_count
    owner_ids = jnp.full((filled,), tok_rows, jnp.int32).at[slot_ids].set(route_owner)
    sent_weights = (
        jnp.zeros((filled,), jnp.bfloat16)
        .at[slot_ids]
        .set(route_weights.reshape(-1).astype(jnp.bfloat16))
    )
    first_col = lax.axis_index("tp") * quarter
    own_rows = lax.dynamic_slice_in_dim(tokens, first_col, quarter, 1)
    own_grads = lax.dynamic_slice_in_dim(cotangent, first_col, quarter, 1)
    sent_rows = jnp.take(own_rows, owner_ids, axis=0, mode="fill", fill_value=0)
    sent_grads = jnp.take(own_grads, owner_ids, axis=0, mode="fill", fill_value=0)
    got_rows, got_grads, got_weights = (
        lax.all_to_all(sent_rows, "ep", split_axis=0, concat_axis=0, tiled=True),
        lax.all_to_all(sent_grads, "ep", split_axis=0, concat_axis=0, tiled=True),
        lax.all_to_all(sent_weights, "ep", split_axis=0, concat_axis=0, tiled=True),
    )
    got_rows, got_grads = (
        lax.all_gather(got_rows, "tp", axis=1, tiled=True),
        lax.all_gather(got_grads, "tp", axis=1, tiled=True),
    )
    slot_rows = got_rows.reshape(ep_size, exp_local, capacity, feat_width)
    slot_grads = got_grads.reshape(ep_size, exp_local, capacity, feat_width)
    weight_col = got_weights.reshape(ep_size, exp_local, capacity, 1).astype(jnp.float32)
    gate = jnp.einsum("secd,edf->secf", slot_rows, gate_proj, preferred_element_type=jnp.float32)
    upper = jnp.einsum("secd,edf->secf", slot_rows, up_proj, preferred_element_type=jnp.float32)
    active = jax.nn.silu(gate)
    hidden = (active * upper).astype(jnp.bfloat16)
    backed = jnp.einsum("secd,efd->secf", slot_grads, down_proj, preferred_element_type=jnp.float32)
    gate_share = jnp.sum(hidden.astype(jnp.float32) * backed, axis=3)
    d_hidden = weight_col * backed
    sigma = jax.nn.sigmoid(gate)
    d_gate = (d_hidden * upper * sigma * (1.0 + gate * (1.0 - sigma))).astype(jnp.bfloat16)
    d_up = (d_hidden * active).astype(jnp.bfloat16)
    scaled = (weight_col * slot_grads).astype(jnp.bfloat16)
    down_proj_grad = jnp.einsum(
        "secf,secd->efd", hidden, scaled, preferred_element_type=jnp.float32
    ).astype(jnp.bfloat16)
    gate_proj_grad = jnp.einsum(
        "secd,secf->edf", slot_rows, d_gate, preferred_element_type=jnp.float32
    ).astype(jnp.bfloat16)
    up_proj_grad = jnp.einsum(
        "secd,secf->edf", slot_rows, d_up, preferred_element_type=jnp.float32
    ).astype(jnp.bfloat16)
    partial_value = jnp.einsum(
        "secf,edf->secd", d_gate, gate_proj, preferred_element_type=jnp.float32
    )
    partial_value = partial_value + jnp.einsum(
        "secf,edf->secd", d_up, up_proj, preferred_element_type=jnp.float32
    )
    gate_whole = lax.psum(gate_share, "tp")
    input_cols = lax.psum_scatter(
        partial_value.astype(jnp.bfloat16), "tp", scatter_dimension=3, tiled=True
    )
    back_cols, back_gate = (
        lax.all_to_all(
            input_cols.reshape(filled, quarter), "ep", split_axis=0, concat_axis=0, tiled=True
        ),
        lax.all_to_all(
            gate_whole.astype(jnp.bfloat16).reshape(filled),
            "ep",
            split_axis=0,
            concat_axis=0,
            tiled=True,
        ),
    )
    picked = back_cols[slot_ids].reshape(tok_rows, top_count, quarter)
    tokens_grad = jnp.sum(picked.astype(jnp.float32), axis=1).astype(jnp.bfloat16)
    weights_grad = back_gate[slot_ids].astype(jnp.float32).reshape(tok_rows, top_count)
    hidden_grad = jnp.dot(cotangent, shared_down, preferred_element_type=jnp.float32).astype(
        jnp.bfloat16
    )
    shared_grad = lax.psum_scatter(
        jnp.einsum("td,th->dh", cotangent, shared_hidden, preferred_element_type=jnp.float32),
        "ep",
        scatter_dimension=0,
        tiled=True,
    )
    return (
        tokens_grad,
        weights_grad,
        gate_proj_grad,
        up_proj_grad,
        down_proj_grad,
        hidden_grad,
        shared_grad,
    )


def solution(mesh):
    in_specs = (
        P("ep", None),
        P("ep", None),
        P("ep", None),
        P("ep", None),
        P("ep", None, "tp"),
        P("ep", None, "tp"),
        P("ep", "tp", None),
        P(None, "tp"),
        P("ep", "tp"),
    )
    out_specs = (
        P("ep", "tp"),
        P("ep", None),
        P("ep", None, "tp"),
        P("ep", None, "tp"),
        P("ep", "tp", None),
        P("ep", "tp"),
        P("ep", "tp"),
    )
    return jax.shard_map(shards, mesh=mesh, in_specs=in_specs, out_specs=out_specs, check_vma=False)
```

```python
import functools

import jax
import jax.numpy as jnp
from jax import lax
from jax.experimental import pallas as pl
from jax.experimental.pallas import tpu as pltpu
from jax.sharding import PartitionSpec as P

MESH = pl.DeviceIdType.MESH
BF = jnp.bfloat16
F32 = jnp.float32
DISP, WGT, FWD_X, FWD_C, FWD_XC, RET_C, RET_X, RET_EP, RET_G, SHARE, GSUM, PAIR = range(12)


def dot_f32(a, b, dims):
    return lax.dot_general(a, b, (dims, ((), ())), preferred_element_type=F32)


def kernel(
    n,
    cap,
    tok_ref,
    cot_ref,
    rw_ref,
    rt_ref,
    wg_ref,
    wu_ref,
    wd_ref,
    sd_ref,
    sh_ref,
    otok_ref,
    ow_ref,
    og_ref,
    ou_ref,
    od_ref,
    ohid_ref,
    osh_ref,
    perm,
    sbuf,
    abuf,
    wsend,
    wrecv,
    wgu,
    wdv,
    sdv,
    gradv,
    hw,
    dgu,
    part,
    crecv,
    keep,
    xsend,
    xrecv,
    rsend,
    ret,
    gpart,
    gcore,
    gtwo,
    gx,
    gsend,
    gret,
    ssend,
    spair,
    ssum,
    srecv,
    send_sem,
    recv_sem,
    load_sem,
    store_sem,
):
    me = lax.axis_index("ep")
    tp = lax.axis_index("tp")
    tok_rows, feat = tok_ref.shape
    top = rt_ref.shape[0]
    quarter = feat // 4
    units = wg_ref.shape[1]
    core_of = lax.rem(tp, 2)
    half_of = tp // 2
    tp_c = half_of * 2 + (1 - core_of)
    tp_x = (1 - half_of) * 2 + core_of
    tp_xc = (1 - half_of) * 2 + (1 - core_of)

    def copy(kind, at, src_ref, dst_ref, ep_to, tp_to):
        return pltpu.make_async_remote_copy(
            src_ref=src_ref,
            dst_ref=dst_ref,
            send_sem=send_sem.at[kind, at],
            recv_sem=recv_sem.at[kind, at],
            device_id=(ep_to, tp_to),
            device_id_type=MESH,
        )

    loads = [
        pltpu.make_async_copy(wg_ref, wgu.at[:, pl.ds(0, units)], load_sem.at[0]),
        pltpu.make_async_copy(wu_ref, wgu.at[:, pl.ds(units, units)], load_sem.at[1]),
        pltpu.make_async_copy(wd_ref, wdv, load_sem.at[2]),
        pltpu.make_async_copy(sd_ref, sdv, load_sem.at[3]),
    ]
    barrier = pltpu.get_barrier_semaphore()
    for d in range(1, n):
        pl.semaphore_signal(
            barrier, inc=1, device_id=(jnp.bitwise_xor(me, d), tp), device_id_type=MESH
        )
    for other in (tp_c, tp_x):
        pl.semaphore_signal(barrier, inc=1, device_id=(me, other), device_id_type=MESH)

    for load in loads:
        load.start()

    names = lax.broadcasted_iota(jnp.int32, (128, tok_rows), 0)
    named_t = jnp.zeros((128, tok_rows), F32)
    weight_t = jnp.zeros((128, tok_rows), F32)
    for k in range(top):
        hit = rt_ref[k : k + 1, :] == names
        named_t = named_t + jnp.where(hit, 1.0, 0.0)
        weight_t = weight_t + jnp.where(hit, rw_ref[k : k + 1, :].astype(BF).astype(F32), 0.0)
    before = lax.broadcasted_iota(jnp.int32, (tok_rows, tok_rows), 0) < lax.broadcasted_iota(
        jnp.int32, (tok_rows, tok_rows), 1
    )
    rank_t = dot_f32(named_t.astype(BF), jnp.where(before, 1.0, 0.0).astype(BF), ((1,), (0,)))
    slot = lax.broadcasted_iota(jnp.int32, (cap, tok_rows), 0).astype(F32)
    wsend[...] = jnp.zeros_like(wsend)
    gpart[...] = jnp.zeros_like(gpart)
    for e in range(n):
        pick = jnp.where(slot == rank_t[e : e + 1, :], named_t[e : e + 1, :], 0.0).astype(BF)
        perm[e] = pick
        wrow = jnp.broadcast_to(weight_t[e : e + 1, :], (8, tok_rows)).astype(BF)
        wsend[e, :, 0:cap] = dot_f32(wrow, pick, ((1,), (1,)))
    every = perm[...].reshape(n * cap, tok_rows)
    cols = pl.ds(pl.multiple_of(tp * quarter, quarter), quarter)
    sbuf[:, 0] = dot_f32(every, tok_ref[:, cols], ((1,), (0,))).astype(BF).reshape(n, cap, quarter)
    sbuf[:, 1] = dot_f32(every, cot_ref[:, cols], ((1,), (0,))).astype(BF).reshape(n, cap, quarter)

    pl.semaphore_wait(barrier, n + 1)

    def disp(d):
        to = jnp.bitwise_xor(me, d)
        return copy(DISP, d, sbuf.at[to], abuf.at[me, tp], to, tp)

    def disp_w(d):
        to = jnp.bitwise_xor(me, d)
        return copy(WGT, d, wsend.at[to], wrecv.at[me], to, tp)

    def disp_in(d):
        of = jnp.bitwise_xor(me, d)
        return copy(DISP, d, abuf.at[of, tp], abuf.at[of, tp], of, tp)

    def disp_w_in(d):
        of = jnp.bitwise_xor(me, d)
        return copy(WGT, d, wrecv.at[of], wrecv.at[of], of, tp)

    def fwd(kind, d, block, to):
        of = jnp.bitwise_xor(me, d)
        return copy(kind, d, abuf.at[of, block], abuf.at[of, block], me, to)

    abuf[me, tp] = sbuf[me]
    wrecv[me] = wsend[me]

    half = n // 2
    for d in [half, half + 1] + list(range(1, half)):
        disp(d).start()
    for d in range(1, n):
        disp_w(d).start()

    for load in loads:
        load.wait()
    ohid_ref[...] = dot_f32(cot_ref[...], sdv[...], ((1,), (0,))).astype(BF)
    rows_each = feat // n
    for j in range(n):
        ssend[j % 2, j // 2] = dot_f32(
            cot_ref[:, j * rows_each : (j + 1) * rows_each], sh_ref[...], ((0,), (0,))
        ).astype(BF)
    odd = lax.rem(me, 2)
    pair = copy(PAIR, 0, ssend.at[1 - odd], spair, jnp.bitwise_xor(me, 1), tp)
    pair.start()

    def share(d):
        to = jnp.bitwise_xor(me, 2 * d)
        return copy(SHARE, d, ssum.at[to // 2], srecv.at[me // 2], to, tp)

    def share_in(d):
        of = jnp.bitwise_xor(me, 2 * d)
        return copy(SHARE, d, srecv.at[of // 2], srecv.at[of // 2], of, tp)

    eye = lax.broadcasted_iota(jnp.int32, (cap, cap), 0) == lax.broadcasted_iota(
        jnp.int32, (cap, cap), 1
    )

    def to_core(d):
        of = jnp.bitwise_xor(me, d)
        return copy(RET_C, d, part.at[of, 1 - core_of], crecv.at[of], me, tp_c)

    def arrive(d):
        @pl.when(d > 0)
        def _():
            disp_in(d).wait_recv()
            disp_w_in(d).wait_recv()

        fwd(FWD_X, d, tp, tp_x).start()
        fwd(FWD_C, d, tp, tp_c).start()

        @pl.when((d >= half) & (d < n - 2))
        def _():
            disp(d).wait_send()
            disp(d + 2).start()

    def pass_core(d):
        fwd(FWD_X, d, tp_x, tp_x).wait_recv()
        fwd(FWD_XC, d, tp_x, tp_c).start()

    def compute(d):
        of = jnp.bitwise_xor(me, d)
        fwd(FWD_C, d, tp_c, tp_c).wait_recv()
        fwd(FWD_XC, d, tp_xc, tp_c).wait_recv()
        both = jnp.zeros((cap, 2 * units), F32)
        backed = jnp.zeros((cap, units), F32)
        for b in range(4):
            at = slice(b * quarter, (b + 1) * quarter)
            both = both + dot_f32(abuf[of, b, 0], wgu[at, :], ((1,), (0,)))
            backed = backed + dot_f32(abuf[of, b, 1], wdv[:, at], ((1,), (1,)))
        gate = both[:, 0:units]
        upper = both[:, units : 2 * units]
        sigma = jax.nn.sigmoid(gate)
        active = gate * sigma
        hidden = (active * upper).astype(BF).astype(F32)
        wcol = jnp.sum(jnp.where(eye, wrecv[of, 0:1, 0:cap], 0.0), axis=1, keepdims=True)
        d_hidden = wcol * backed
        hw[of] = (wcol * hidden).astype(BF)
        d_both = jnp.concatenate(
            [
                (d_hidden * upper * sigma * (1.0 + gate * (1.0 - sigma))).astype(BF),
                (d_hidden * active).astype(BF),
            ],
            axis=1,
        )
        dgu[of] = d_both
        gpart[of, :, 0:cap] = lax.dot_general(
            jnp.ones((8, units), F32),
            hidden * backed,
            (((1,), (1,)), ((), ())),
            precision=lax.Precision.HIGHEST,
            preferred_element_type=F32,
        )
        for b in range(4):
            at = slice(b * quarter, (b + 1) * quarter)
            part[of, b % 2, b // 2] = dot_f32(d_both, wgu[at, :], ((1,), (1,))).astype(BF)
        to_core(d).start()

    def gate_copy(at, src_ref, dst_ref, to):
        return copy(GSUM, at, src_ref, dst_ref, me, to)

    def to_x(d):
        of = jnp.bitwise_xor(me, d)
        return copy(RET_X, d, xsend.at[of], xrecv.at[of], me, tp_x)

    def core_sum(d):
        of = jnp.bitwise_xor(me, d)
        to_core(d).wait_recv()
        xsend[of] = (
            part[of, core_of, 1 - half_of].astype(F32) + crecv[of, 1 - half_of].astype(F32)
        ).astype(BF)
        to_x(d).start()
        keep[of] = part[of, core_of, half_of].astype(F32) + crecv[of, half_of].astype(F32)

    def back(d):
        to = jnp.bitwise_xor(me, d)
        return copy(RET_EP, d, rsend.at[to], ret.at[me], to, tp)

    def back_g(d):
        to = jnp.bitwise_xor(me, d)
        return copy(RET_G, d, gsend.at[to], gret.at[me], to, tp)

    def back_in(d):
        of = jnp.bitwise_xor(me, d)
        return copy(RET_EP, d, ret.at[of], ret.at[of], of, tp)

    def back_g_in(d):
        of = jnp.bitwise_xor(me, d)
        return copy(RET_G, d, gret.at[of], gret.at[of], of, tp)

    def return_block(d):
        of = jnp.bitwise_xor(me, d)
        to_x(d).wait_recv()
        total = (keep[of] + xrecv[of].astype(F32)).astype(BF)

        @pl.when(d == 0)
        def _():
            ret[me] = total

        @pl.when(d > 0)
        def _():
            rsend[of] = total
            back(d).start()

    lag = 4

    @pl.loop(0, n + 2)
    def _(t):
        @pl.when(t < n)
        def _():
            arrive(t)

        @pl.when((t >= 1) & (t <= n))
        def _():
            compute(t - 1)

        @pl.when(t >= 2)
        def _():
            core_sum(t - 2)

        @pl.when(t >= lag)
        def _():
            return_block(t - lag)

        @pl.when(t < n)
        def _():
            pass_core(t)

        @pl.when(t == half)
        def _():
            pair.wait_recv()
            for z in range(half):
                ssum[z] = (ssend[odd, z].astype(F32) + spair[z].astype(F32)).astype(BF)
            srecv[me // 2] = ssum[me // 2]

        @pl.when(t == n - 1)
        def _():
            for other in range(1, half):
                share(other).start()

    gate_copy(0, gpart, gcore, tp_c).start()
    gate_copy(0, gpart, gcore, tp_c).wait()
    gtwo[...] = gpart[...] + gcore[...]
    gate_copy(1, gtwo, gx, tp_x).start()

    d_all = dgu[...].reshape(n * cap, 2 * units)
    h_all = hw[...].reshape(n * cap, units)
    for b in range(4):
        at = slice(b * quarter, (b + 1) * quarter)
        grad = dot_f32(abuf[:, b, 0].reshape(n * cap, quarter), d_all, ((0,), (0,))).astype(BF)
        gradv[0, at, :] = grad[:, 0:units]
        gradv[1, at, :] = grad[:, units : 2 * units]
        wdv[:, at] = dot_f32(
            h_all, abuf[:, b, 1].reshape(n * cap, quarter), ((0,), (0,))
        ).astype(BF)

    stores = [
        pltpu.make_async_copy(gradv.at[0], og_ref, store_sem.at[0]),
        pltpu.make_async_copy(gradv.at[1], ou_ref, store_sem.at[1]),
        pltpu.make_async_copy(wdv, od_ref, store_sem.at[2]),
    ]
    for store in stores:
        store.start()

    gate_copy(1, gtwo, gx, tp_x).wait()
    gsend[...] = gtwo[...] + gx[...]
    gret[me] = gsend[me]

    @pl.loop(1, n)
    def _(d):
        back_g(d).start()

    for d in range(n + 2 - lag, n):
        return_block(jnp.int32(d))

    @pl.loop(1, n)
    def _(d):
        back_g_in(d).wait_recv()

    for d in range(1, half):
        share_in(d).wait_recv()

    sums = srecv[0].astype(F32)
    for j in range(1, half):
        sums = sums + srecv[j].astype(F32)
    osh_ref[...] = sums

    pieces = []
    for e in range(n):
        row = gret[e, :, 0:cap].astype(BF)
        pieces.append(dot_f32(row, perm[e], ((1,), (0,)))[0:1, :])
    pieces.append(jnp.zeros((128 - n, tok_rows), F32))
    values = jnp.concatenate(pieces, axis=0)
    for k in range(top):
        hit = rt_ref[k : k + 1, :] == names
        ow_ref[k : k + 1, :] = jnp.sum(jnp.where(hit, values, 0.0), axis=0, keepdims=True)

    @pl.loop(1, n)
    def _(d):
        back_in(d).wait_recv()

    otok_ref[...] = dot_f32(
        perm[...].reshape(n * cap, tok_rows), ret[...].reshape(n * cap, quarter), ((0,), (0,))
    ).astype(BF)

    for store in stores:
        store.wait()

    @pl.loop(0, n)
    def _(d):
        fwd(FWD_X, d, tp, tp_x).wait_send()
        fwd(FWD_C, d, tp, tp_c).wait_send()
        fwd(FWD_XC, d, tp_x, tp_c).wait_send()
        to_core(d).wait_send()
        to_x(d).wait_send()

    @pl.loop(1, n)
    def _(d):
        back(d).wait_send()
        back_g(d).wait_send()
        disp_w(d).wait_send()

    for d in list(range(1, half)) + [n - 2, n - 1]:
        disp(d).wait_send()
    for d in range(1, half):
        share(d).wait_send()
    pair.wait_send()


def pass_on(*refs):
    count = (len(refs) - 2) // 3
    ins, outs, held = refs[:count], refs[count : 2 * count], refs[2 * count : 3 * count]
    in_sem, out_sem = refs[-2:]
    loads = [pltpu.make_async_copy(ins[i], held[i], in_sem.at[i]) for i in range(count)]
    stores = [pltpu.make_async_copy(held[i], outs[i], out_sem.at[i]) for i in range(count)]
    for load in loads:
        load.start()
    for load, store in zip(loads, stores):
        load.wait()
        store.start()
    for store in stores:
        store.wait()


def hand_over(arrays):
    count = len(arrays)
    hbm = pl.BlockSpec(memory_space=pl.ANY)
    return pl.pallas_call(
        pass_on,
        out_shape=tuple(jax.ShapeDtypeStruct(a.shape, a.dtype) for a in arrays),
        in_specs=[hbm] * count,
        out_specs=tuple([hbm] * count),
        scratch_shapes=[pltpu.VMEM(a.shape, a.dtype) for a in arrays]
        + [pltpu.SemaphoreType.DMA((count,))] * 2,
    )(*arrays)


def fused_shards(
    tokens,
    cotangent,
    route_weights,
    routes,
    gate_proj,
    up_proj,
    down_proj,
    shared_down,
    shared_hidden,
):
    n = lax.axis_size("ep")
    tok_rows, feat = tokens.shape
    units = gate_proj.shape[2]
    hid = shared_hidden.shape[1]
    cap = 2 * tok_rows * routes.shape[1] // n
    quarter = feat // 4
    out_shape = (
        jax.ShapeDtypeStruct((tok_rows, quarter), BF),
        jax.ShapeDtypeStruct(routes.shape[::-1], F32),
        jax.ShapeDtypeStruct((feat, units), BF),
        jax.ShapeDtypeStruct((feat, units), BF),
        jax.ShapeDtypeStruct((units, feat), BF),
        jax.ShapeDtypeStruct((tok_rows, hid), BF),
        jax.ShapeDtypeStruct((feat // n, hid), F32),
    )
    tiles = pltpu.VMEM((n, 8, 128), F32)
    vmem = pl.BlockSpec(memory_space=pltpu.VMEM)
    hbm = pl.BlockSpec(memory_space=pl.ANY)
    outs = pl.pallas_call(
        functools.partial(kernel, n, cap),
        out_shape=out_shape,
        in_specs=[vmem] * 4 + [hbm] * 4 + [vmem],
        out_specs=(vmem, vmem, hbm, hbm, hbm, vmem, vmem),
        scratch_shapes=[
            pltpu.VMEM((n, cap, tok_rows), BF),
            pltpu.VMEM((n, 2, cap, quarter), BF),
            pltpu.VMEM((n, 4, 2, cap, quarter), BF),
            tiles,
            tiles,
            pltpu.VMEM((feat, 2 * units), BF),
            pltpu.VMEM((units, feat), BF),
            pltpu.VMEM((feat, hid), BF),
            pltpu.VMEM((2, feat, units), BF),
            pltpu.VMEM((n, cap, units), BF),
            pltpu.VMEM((n, cap, 2 * units), BF),
            pltpu.VMEM((n, 2, 2, cap, quarter), BF),
            pltpu.VMEM((n, 2, cap, quarter), BF),
            pltpu.VMEM((n, cap, quarter), F32),
            pltpu.VMEM((n, cap, quarter), BF),
            pltpu.VMEM((n, cap, quarter), BF),
            pltpu.VMEM((n, cap, quarter), BF),
            pltpu.VMEM((n, cap, quarter), BF),
            tiles,
            tiles,
            tiles,
            tiles,
            tiles,
            tiles,
            pltpu.VMEM((2, n // 2, feat // n, hid), BF),
            pltpu.VMEM((n // 2, feat // n, hid), BF),
            pltpu.VMEM((n // 2, feat // n, hid), BF),
            pltpu.VMEM((n // 2, feat // n, hid), BF),
            pltpu.SemaphoreType.DMA((12, n)),
            pltpu.SemaphoreType.DMA((12, n)),
            pltpu.SemaphoreType.DMA((4,)),
            pltpu.SemaphoreType.DMA((3,)),
        ],
        compiler_params=pltpu.CompilerParams(
            collective_id=0, has_side_effects=True, vmem_limit_bytes=60 * 1024 * 1024
        ),
    )(
        tokens,
        cotangent,
        route_weights.T,
        routes.T,
        gate_proj[0],
        up_proj[0],
        down_proj[0],
        shared_down,
        shared_hidden,
    )
    outs = hand_over(outs)
    return outs[0], outs[1].T, outs[2][None], outs[3][None], outs[4][None], outs[5], outs[6]


def shards(*args):
    tokens, routes, gate_proj = args[0], args[3], args[4]
    n = lax.axis_size("ep")
    tok_rows, feat = tokens.shape
    fits = (
        gate_proj.shape[0] == 1
        and lax.axis_size("tp") == 4
        and tok_rows == 128
        and n in (8, 16)
        and (2 * tok_rows * routes.shape[1]) % (16 * n) == 0
        and 2 * tok_rows * routes.shape[1] // n <= 128
        and feat % 512 == 0
        and feat // n % 128 == 0
    )
    if fits:
        return fused_shards(*args)
    return plain_shards(*args)


def plain_shards(
    tokens,
    cotangent,
    route_weights,
    routes,
    gate_proj,
    up_proj,
    down_proj,
    shared_down,
    shared_hidden,
):
    tok_rows, feat_width = tokens.shape
    top_count = routes.shape[1]
    exp_local = gate_proj.shape[0]
    ep_size = lax.axis_size("ep")
    tp_size = lax.axis_size("tp")
    exp_total = exp_local * ep_size
    capacity = 2 * tok_rows * top_count // exp_total
    quarter = feat_width // tp_size
    filled = exp_total * capacity
    flat_routes = routes.reshape(-1)
    one_hot = (flat_routes[:, None] == jnp.arange(exp_total, dtype=jnp.int32)[None, :]).astype(
        jnp.int32
    )
    rank_in = jnp.sum((jnp.cumsum(one_hot, axis=0) - one_hot) * one_hot, axis=1)
    slot_ids = flat_routes * capacity + rank_in
    route_owner = jnp.arange(flat_routes.shape[0], dtype=jnp.int32) // top_count
    owner_ids = jnp.full((filled,), tok_rows, jnp.int32).at[slot_ids].set(route_owner)
    sent_weights = (
        jnp.zeros((filled,), jnp.bfloat16)
        .at[slot_ids]
        .set(route_weights.reshape(-1).astype(jnp.bfloat16))
    )
    first_col = lax.axis_index("tp") * quarter
    own_rows = lax.dynamic_slice_in_dim(tokens, first_col, quarter, 1)
    own_grads = lax.dynamic_slice_in_dim(cotangent, first_col, quarter, 1)
    sent_rows = jnp.take(own_rows, owner_ids, axis=0, mode="fill", fill_value=0)
    sent_grads = jnp.take(own_grads, owner_ids, axis=0, mode="fill", fill_value=0)
    got_rows, got_grads, got_weights = (
        lax.all_to_all(sent_rows, "ep", split_axis=0, concat_axis=0, tiled=True),
        lax.all_to_all(sent_grads, "ep", split_axis=0, concat_axis=0, tiled=True),
        lax.all_to_all(sent_weights, "ep", split_axis=0, concat_axis=0, tiled=True),
    )
    got_rows, got_grads = (
        lax.all_gather(got_rows, "tp", axis=1, tiled=True),
        lax.all_gather(got_grads, "tp", axis=1, tiled=True),
    )
    slot_rows = got_rows.reshape(ep_size, exp_local, capacity, feat_width)
    slot_grads = got_grads.reshape(ep_size, exp_local, capacity, feat_width)
    weight_col = got_weights.reshape(ep_size, exp_local, capacity, 1).astype(jnp.float32)
    gate = jnp.einsum("secd,edf->secf", slot_rows, gate_proj, preferred_element_type=jnp.float32)
    upper = jnp.einsum("secd,edf->secf", slot_rows, up_proj, preferred_element_type=jnp.float32)
    active = jax.nn.silu(gate)
    hidden = (active * upper).astype(jnp.bfloat16)
    backed = jnp.einsum("secd,efd->secf", slot_grads, down_proj, preferred_element_type=jnp.float32)
    gate_share = jnp.sum(hidden.astype(jnp.float32) * backed, axis=3)
    d_hidden = weight_col * backed
    sigma = jax.nn.sigmoid(gate)
    d_gate = (d_hidden * upper * sigma * (1.0 + gate * (1.0 - sigma))).astype(jnp.bfloat16)
    d_up = (d_hidden * active).astype(jnp.bfloat16)
    scaled = (weight_col * slot_grads).astype(jnp.bfloat16)
    down_proj_grad = jnp.einsum(
        "secf,secd->efd", hidden, scaled, preferred_element_type=jnp.float32
    ).astype(jnp.bfloat16)
    gate_proj_grad = jnp.einsum(
        "secd,secf->edf", slot_rows, d_gate, preferred_element_type=jnp.float32
    ).astype(jnp.bfloat16)
    up_proj_grad = jnp.einsum(
        "secd,secf->edf", slot_rows, d_up, preferred_element_type=jnp.float32
    ).astype(jnp.bfloat16)
    partial_value = jnp.einsum(
        "secf,edf->secd", d_gate, gate_proj, preferred_element_type=jnp.float32
    )
    partial_value = partial_value + jnp.einsum(
        "secf,edf->secd", d_up, up_proj, preferred_element_type=jnp.float32
    )
    gate_whole = lax.psum(gate_share, "tp")
    input_cols = lax.psum_scatter(
        partial_value.astype(jnp.bfloat16), "tp", scatter_dimension=3, tiled=True
    )
    back_cols, back_gate = (
        lax.all_to_all(
            input_cols.reshape(filled, quarter), "ep", split_axis=0, concat_axis=0, tiled=True
        ),
        lax.all_to_all(
            gate_whole.astype(jnp.bfloat16).reshape(filled),
            "ep",
            split_axis=0,
            concat_axis=0,
            tiled=True,
        ),
    )
    picked = back_cols[slot_ids].reshape(tok_rows, top_count, quarter)
    tokens_grad = jnp.sum(picked.astype(jnp.float32), axis=1).astype(jnp.bfloat16)
    weights_grad = back_gate[slot_ids].astype(jnp.float32).reshape(tok_rows, top_count)
    hidden_grad = jnp.dot(cotangent, shared_down, preferred_element_type=jnp.float32).astype(
        jnp.bfloat16
    )
    shared_grad = lax.psum_scatter(
        jnp.einsum("td,th->dh", cotangent, shared_hidden, preferred_element_type=jnp.float32),
        "ep",
        scatter_dimension=0,
        tiled=True,
    )
    return (
        tokens_grad,
        weights_grad,
        gate_proj_grad,
        up_proj_grad,
        down_proj_grad,
        hidden_grad,
        shared_grad,
    )


def solution(mesh):
    in_specs = (
        P("ep", None),
        P("ep", None),
        P("ep", None),
        P("ep", None),
        P("ep", None, "tp"),
        P("ep", None, "tp"),
        P("ep", "tp", None),
        P(None, "tp"),
        P("ep", "tp"),
    )
    out_specs = (
        P("ep", "tp"),
        P("ep", None),
        P("ep", None, "tp"),
        P("ep", None, "tp"),
        P("ep", "tp", None),
        P("ep", "tp"),
        P("ep", "tp"),
    )
    return jax.shard_map(shards, mesh=mesh, in_specs=in_specs, out_specs=out_specs, check_vma=False)
```
